512 devices in a mesh: ep: 128 (over z, y, core), tp: 4 (over x).
Axes of the slice: x: 4, y: 8, z: 8, core: 2. Of those that a mesh axis runs over, the one named last changes fastest.
Arguments:
- tokens: bfloat16 [2048, 2048], P('ep'), may hold values from -6 to 6
- head_state: float32 [2048, 16, 4096], P('ep', 'tp'), may hold values from -6 to 6
- mixer_gain: float32 [2048], replicated, may hold values from 0.1 to 1.9
- w_query: bfloat16 [2048, 1024], P('ep', 'tp'), may hold values from -0.125 to 0.125
- w_key: bfloat16 [2048, 1024], P('ep', 'tp'), may hold values from -0.125 to 0.125
- w_value: bfloat16 [2048, 1024], P('ep', 'tp'), may hold values from -0.125 to 0.125
- decay_down: bfloat16 [2048, 64], replicated, may hold values from -0.125 to 0.125
- decay_up: bfloat16 [64, 1024], replicated, may hold values from -3 to 3
- decay_base: float32 [1024], P('tp'), may hold values from -4 to 0
- rate_down: bfloat16 [2048, 64], replicated, may hold values from -0.125 to 0.125
- rate_up: bfloat16 [64, 1024], replicated, may hold values from -0.75 to 0.75
- head_gain: float32 [1024], P('tp'), may hold values from 0.1 to 1.9
- w_out: bfloat16 [1024, 2048], P('tp', 'ep'), may hold values from -0.1875 to 0.1875
- expert_gain: float32 [2048], replicated, may hold values from 0.1 to 1.9
- expert_ids: int32 [2048, 2], P('ep'), may hold values from 0 to 127, all different within a row; in each aligned block of 16 rows (0 to 15, 16 to 31, ...) at most 1 rows name the same one
- route_weight: float32 [2048, 2], P('ep'), may hold values from 0.2 to 1
- w_gate: bfloat16 [128, 2048, 512], P('ep', None, 'tp'), may hold values from -0.125 to 0.125
- w_up: bfloat16 [128, 2048, 512], P('ep', None, 'tp'), may hold values from -0.125 to 0.125
- w_down: bfloat16 [128, 512, 2048], P('ep', 'tp'), may hold values from -0.25 to 0.25
Outputs:
- layer_out: bfloat16 [2048, 2048], P('ep', 'tp')
- next_state: float32 [2048, 16, 4096], P('ep', 'tp')
The draws below stay inside these ranges and needn't reach their ends.
Inputs may be any that keep to these rules, and one draw needn't show every extreme that they name: `expert_ids`: each row names 2 different experts; among the 16 rows of one index of ep no expert is named more than 1 times, and in the rows of some indices one expert is named exactly 1 times.
All inputs are finite; a program needn't handle non-finite values.
Results may differ from the reference program's by a relative error of at most 0.015.
Values may be sent and summed in bfloat16 or wider, within the bound.
A program may use at most 64 MiB of HBM per device.

```python
import math
import jax
import jax.numpy as jnp
import numpy as np
from jax import lax

D = 2048
HEADS = 16
HS = 64
RANK = 64
FF = 512
TOP_K = 2
SEQ_DEV = 16
D_A = 1024
TOKENS = 2048
EXPERTS = 128
CAP = 1
N_EP = 128


def level_of(key, dims, pieces, smallest, top_value):
    def one(position, shards_of):
        draws = jax.random.uniform(jax.random.fold_in(jax.random.fold_in(key, 6), position), (shards_of,), jnp.float32, smallest / len(pieces), top_value / len(pieces))
        return jnp.repeat(jnp.exp(draws), dims[position] // shards_of).reshape((-1,) + (1,) * (len(dims) - position - 1))

    level = one(*pieces[0])
    for cut in pieces[1:]:
        level = level * one(*cut)
    return level


def assign_block(stream_key, own, number, rows, count, top, most, lean):
    ranking = jax.random.permutation(stream_key, count)
    packed, ordinary = load_shares(count, rows * top, most, lean, True), load_shares(count, rows * top, most, lean, False)
    places = jnp.arange(count)

    def named(sizes, offset_by):
        used = int((sizes > 0).sum())
        fixed = max(1, used // 4)
        passed = fixed + (places - fixed + offset_by * (used - fixed)) % max(1, count - fixed)
        return jnp.zeros((count,), jnp.int32).at[ranking[jnp.where(places < fixed, places, passed)]].set(jnp.asarray(sizes, jnp.int32))

    sizes = jnp.where(number % 4 == 0, named(packed, number // 4), named(ordinary, number - number // 4 - 1))
    mixed = jax.random.permutation(jax.random.fold_in(own, 3), count)
    giver, receiver = mixed[0:count // 2 * 2:2], mixed[1:count // 2 * 2:2]
    margin = jnp.minimum(sizes[giver] - 1, most - sizes[receiver]) // 2
    margin = jnp.where((giver == ranking[0]) | (receiver == ranking[0]) | (sizes[receiver] == 0), 0, jnp.maximum(margin, 0))
    passed = jax.random.randint(jax.random.fold_in(own, 4), (count // 2,), 0, 1 << 20) % (margin + 1)
    sizes = sizes.at[giver].add(-passed).at[receiver].add(passed)
    labels = jnp.searchsorted(jnp.cumsum(sizes), jnp.arange(rows * top), side="right").astype(jnp.int32)
    listing = labels.reshape(top, rows).T
    listing = listing[jax.random.permutation(jax.random.fold_in(own, 1), rows)]
    offset_by = jax.random.randint(jax.random.fold_in(own, 2), (rows, 1), 0, top)
    return jnp.take_along_axis(listing, (jnp.arange(top)[None, :] + offset_by) % top, axis=1)


def load_shares(amount, total, reach, skew, full):
    weights = [(1 << 20) // math.isqrt(standing ** skew) + 1 for standing in range(1, amount + 1)]
    largest = reach if full else min(reach, max(-(-total // amount), total * weights[0] // sum(weights)))
    least = 1 if total - largest >= amount - 1 else 0
    counts, spare = [largest] + [least] * (amount - 1), total - largest - least * (amount - 1)
    while spare > 0:
        free = [i for i in range(1, amount) if counts[i] < largest] or [i for i in range(1, amount) if counts[i] < reach]
        whole, budget = sum([weights[i] for i in free]), spare
        for i in free:
            addition = min(reach - counts[i], max(1, budget * weights[i] // whole), spare)
            counts[i] = counts[i] + addition
            spare = spare - addition
    return np.array(counts)


def gaussian(stream_key, dims, scale, limit, shards=(), kind=jnp.bfloat16):
    drawn = scale * jax.random.normal(stream_key, dims, jnp.float32)
    if shards:
        drawn = drawn * level_of(stream_key, dims, shards, -0.22, 0.18)
    return jnp.clip(drawn, -limit, limit).astype(kind)


def setup_inputs(seed: int = 0) -> dict:
    splits = jax.random.split(jax.random.key(seed), 20)
    tokens = gaussian(splits[0], (TOKENS, D), 1.0, 6.0, ((0, 128),))
    head_state = gaussian(splits[1], (TOKENS, HEADS, HS * HS), 1.0, 6.0, ((0, 128), (1, 4)), jnp.float32)
    mixer_gain = jnp.clip(1.0 + 0.18 * jax.random.normal(splits[2], (D,), jnp.float32), 0.1, 1.9)
    w_query = gaussian(splits[3], (D, D_A), D ** -0.5, 0.125, ((0, 128), (1, 4)))
    w_key = gaussian(splits[4], (D, D_A), D ** -0.5, 0.125, ((0, 128), (1, 4)))
    w_value = gaussian(splits[5], (D, D_A), D ** -0.5, 0.125, ((0, 128), (1, 4)))
    decay_down = gaussian(splits[6], (D, RANK), D ** -0.5, 0.125)
    decay_up = gaussian(splits[7], (RANK, D_A), 0.5, 3.0)
    decay_base = jnp.clip(-4.0 + 4.0 * jax.random.uniform(splits[8], (D_A,), jnp.float32) ** level_of(splits[8], (D_A,), ((0, 4),), -0.2, 0.2), -4.0, 0.0)
    rate_down = gaussian(splits[9], (D, RANK), D ** -0.5, 0.125)
    rate_up = gaussian(splits[10], (RANK, D_A), RANK ** -0.5, 0.75)
    head_gain = jnp.clip(1.0 + 0.18 * jax.random.normal(splits[11], (D_A,), jnp.float32), 0.1, 1.9)
    w_out = gaussian(splits[12], (D_A, D), D_A ** -0.5, 0.1875, ((0, 4), (1, 128)))
    expert_gain = jnp.clip(1.0 + 0.18 * jax.random.normal(splits[13], (D,), jnp.float32), 0.1, 1.9)
    expert_ids_keys = jax.random.split(jax.random.fold_in(splits[14], 1), TOKENS // SEQ_DEV)
    expert_ids_turns = jax.random.permutation(jax.random.fold_in(splits[14], 3), TOKENS // SEQ_DEV)
    expert_ids = jax.vmap(lambda own, number: assign_block(jax.random.fold_in(splits[14], 2), own, number, SEQ_DEV, EXPERTS, TOP_K, CAP, 2))(expert_ids_keys, expert_ids_turns).reshape((TOKENS, TOP_K))
    route_weight = jnp.clip(jnp.exp(math.log(1.0) - 1.609438 * jax.random.uniform(splits[15], (TOKENS, TOP_K), jnp.float32) ** level_of(splits[15], (TOKENS, TOP_K), ((0, 128),), -0.2, 0.2)), 0.2, 1.0)
    w_gate = gaussian(splits[16], (EXPERTS, D, FF), D ** -0.5, 0.125, ((0, 128), (2, 4)))
    w_up = gaussian(splits[17], (EXPERTS, D, FF), D ** -0.5, 0.125, ((0, 128), (2, 4)))
    w_down = gaussian(splits[18], (EXPERTS, FF, D), FF ** -0.5, 0.25, ((0, 128), (1, 4)))
    return {"tokens": tokens, "head_state": head_state, "mixer_gain": mixer_gain, "w_query": w_query, "w_key": w_key, "w_value": w_value, "decay_down": decay_down, "decay_up": decay_up, "decay_base": decay_base, "rate_down": rate_down, "rate_up": rate_up, "head_gain": head_gain, "w_out": w_out, "expert_gain": expert_gain, "expert_ids": expert_ids, "route_weight": route_weight, "w_gate": w_gate, "w_up": w_up, "w_down": w_down}


norm_eps = 1e-06
group_eps = 0.00064

def rms_scale(activity, gain):
    widened = activity.astype(jnp.float32)
    scaled = widened * lax.rsqrt(lax.optimization_barrier(jnp.mean(widened * widened, axis=-1, keepdims=True)) + norm_eps)
    return (scaled * gain).astype(jnp.bfloat16)

def low_rank(normed, decay_down, decay_up, decay_base, rate_down, rate_up):
    decay_low = jnp.tanh(jnp.dot(normed, decay_down, preferred_element_type=jnp.float32)).astype(jnp.bfloat16)
    decay_pre = decay_base + jnp.dot(decay_low, decay_up, preferred_element_type=jnp.float32)
    decays = jnp.exp(-jnp.exp(-jax.nn.softplus(-decay_pre) - 0.5))
    rate_low = jnp.dot(normed, rate_down, preferred_element_type=jnp.float32).astype(jnp.bfloat16)
    rates = jax.nn.sigmoid(jnp.dot(rate_low, rate_up, preferred_element_type=jnp.float32))
    return (decays, rates)

def recurrence(queries, key_rows, value_rows, decays, rates, old_state, head_gain):
    row_count, head_count, _ = old_state.shape
    head_size = queries.shape[1] // head_count
    head_shape = (row_count, head_count, head_size)
    query_heads = queries.astype(jnp.float32).reshape(head_shape)
    key_heads = key_rows.astype(jnp.float32).reshape(head_shape)
    value_heads = value_rows.astype(jnp.float32).reshape(head_shape)
    decay_heads = decays.reshape(head_shape)
    rate_heads = rates.reshape(head_shape)
    unit_keys = key_heads * lax.rsqrt(lax.optimization_barrier(jnp.sum(key_heads * key_heads, axis=-1, keepdims=True)) + 1.0)
    state_grid = old_state.reshape(row_count, head_count, head_size, head_size)
    removed = lax.optimization_barrier(jnp.sum(state_grid * unit_keys[:, :, None, :], axis=-1))
    updated = state_grid * decay_heads[:, :, None, :] - removed[:, :, :, None] * (unit_keys * rate_heads)[:, :, None, :] + value_heads[:, :, :, None] * key_heads[:, :, None, :]
    readout = lax.optimization_barrier(jnp.sum(updated * query_heads[:, :, None, :], axis=-1))
    centred = readout - lax.optimization_barrier(jnp.mean(readout, axis=-1, keepdims=True))
    spread = lax.optimization_barrier(jnp.mean(centred * centred, axis=-1, keepdims=True))
    scaled = centred * lax.rsqrt(spread + group_eps) * head_gain.reshape(head_count, head_size)
    return (updated.reshape(row_count, head_count, head_size * head_size), scaled.reshape(row_count, head_count * head_size).astype(jnp.bfloat16))

def reference(tokens, head_state, mixer_gain, w_query, w_key, w_value, decay_down, decay_up, decay_base, rate_down, rate_up, head_gain, w_out, expert_gain, expert_ids, route_weight, w_gate, w_up, w_down):
    normed = rms_scale(tokens, mixer_gain)
    queries = jnp.dot(normed, w_query, preferred_element_type=jnp.float32).astype(jnp.bfloat16)
    key_rows = jnp.dot(normed, w_key, preferred_element_type=jnp.float32).astype(jnp.bfloat16)
    value_rows = jnp.dot(normed, w_value, preferred_element_type=jnp.float32).astype(jnp.bfloat16)
    decays, rates = low_rank(normed, decay_down, decay_up, decay_base, rate_down, rate_up)
    next_state, head_out = recurrence(queries, key_rows, value_rows, decays, rates, head_state, head_gain)
    mixed_out = jnp.dot(head_out, w_out, preferred_element_type=jnp.float32)
    residual = (tokens.astype(jnp.float32) + mixed_out).astype(jnp.bfloat16)
    expert_in = rms_scale(residual, expert_gain)
    top_count = expert_ids.shape[1]
    flat_ids = expert_ids.reshape(-1).astype(jnp.int32)
    pair_count = flat_ids.shape[0]
    shares = (route_weight / lax.optimization_barrier(jnp.sum(route_weight, axis=1, keepdims=True))).reshape(-1)
    buffer_rows = N_EP * CAP
    positions = jnp.arange(pair_count, dtype=jnp.int32)

    def one_expert(running, inputs):
        expert, gate_local, up_local, down_local = inputs
        matches = flat_ids == expert
        order_keys = jnp.where(matches, positions, positions + pair_count)
        chosen = jnp.argsort(order_keys)[:buffer_rows].astype(jnp.int32)
        in_range = jnp.arange(buffer_rows, dtype=jnp.int32) < jnp.sum(matches.astype(jnp.int32))
        owners = (chosen // top_count).astype(jnp.int32)
        picked = expert_in[owners]
        gate_act = jnp.dot(picked, gate_local, preferred_element_type=jnp.float32)
        up_act = jnp.dot(picked, up_local, preferred_element_type=jnp.float32)
        hidden = (jax.nn.silu(gate_act) * up_act).astype(jnp.bfloat16)
        result = jnp.dot(hidden, down_local, preferred_element_type=jnp.float32).astype(jnp.bfloat16)
        weights = jnp.where(in_range, shares[chosen], 0.0)
        running = running.at[owners].add(weights[:, None] * result.astype(jnp.float32))
        return (running, None)
    zero_sums = jnp.zeros(expert_in.shape, jnp.float32)
    routed, _ = lax.scan(one_expert, zero_sums, (jnp.arange(EXPERTS, dtype=jnp.int32), w_gate, w_up, w_down))
    layer_out = (residual.astype(jnp.float32) + routed).astype(jnp.bfloat16)
    return (layer_out, next_state)
```

```python
import jax
import jax.numpy as jnp
from jax import lax
from jax.experimental import pallas as pl
from jax.experimental.pallas import tpu as pltpu
from jax.sharding import PartitionSpec as P

norm_eps = 1e-06
group_eps = 0.00064

MESH = pl.DeviceIdType.MESH


def offset_at(i):
    return ((i + 1) // 2) * (2 * (i % 2) - 1)


def gather_kernel(wq, wk, wv, wo, out, own_sem, send_sem, recv_sem):
    ep = lax.axis_index("ep")
    core = ep % 2
    y = (ep // 2) % 8
    z = ep // 16
    a = z + core * (y - z)
    b = y + core * (z - y)
    partner = ep + 1 - 2 * core

    def at(da, db):
        aa = (a + da + 8) % 8
        bb = (b + db + 8) % 8
        return aa * (16 - 14 * core) + bb * (2 + 14 * core) + core

    barrier = pltpu.get_barrier_semaphore()
    for i in range(1, 8):
        pl.semaphore_signal(barrier, inc=1, device_id={"ep": at(offset_at(i), 0)}, device_id_type=MESH)
    pl.semaphore_signal(barrier, inc=1, device_id={"ep": at(0, 1)}, device_id_type=MESH)
    pl.semaphore_signal(barrier, inc=1, device_id={"ep": at(0, -1)}, device_id_type=MESH)
    pl.semaphore_signal(barrier, inc=1, device_id={"ep": partner}, device_id_type=MESH)

    own = [
        pltpu.make_async_copy(w, out.at[m, ep], own_sem.at[m]) for m, w in enumerate((wq, wk, wv, wo))
    ]
    for copy in own:
        copy.start()
    for copy in own:
        copy.wait()
    pl.semaphore_wait(barrier, 10)

    def copy_of(block, slot, to):
        return pltpu.make_async_remote_copy(
            src_ref=out.at[:, block],
            dst_ref=out.at[:, block],
            send_sem=send_sem.at[slot],
            recv_sem=recv_sem.at[block],
            device_id={"ep": to},
            device_id_type=MESH,
        )

    def send(block, slot, to):
        copy_of(block, slot, to).start()

    def arrived(block):
        copy_of(block, 0, partner).wait_recv()

    forth = at(0, 1)
    back = at(0, -1)

    @pl.loop(1, 8)
    def _(i):
        send(ep, i, at(offset_at(i), 0))

    @pl.loop(0, 8)
    def _(i):
        block = at(offset_at(i), 0)

        @pl.when(i > 0)
        def _():
            arrived(block)

        send(block, 8 + i, forth)
        send(block, 36 + i, back)
        send(block, 64 + i, partner)

    @pl.loop(1, 3)
    def _(s):
        @pl.loop(0, 8)
        def _(i):
            o = offset_at(i)
            left = at(o, -s)
            arrived(left)
            send(left, 8 + 8 * s + i, forth)
            send(left, 64 + 16 * s - 8 + i, partner)
            right = at(o, s)
            arrived(right)
            send(right, 36 + 8 * s + i, back)
            send(right, 64 + 16 * s + i, partner)

    @pl.loop(0, 4)
    def _(h):
        for d in range(2):
            i = 2 * h + d
            o = offset_at(i)
            left = at(o, -3)
            arrived(left)
            if d == 0:
                send(left, 8 + 24 + h, forth)
            send(left, 64 + 40 + i, partner)
            right = at(o, 3)
            arrived(right)
            if d == 1:
                send(right, 36 + 24 + h, back)
            send(right, 64 + 48 + i, partner)

    @pl.loop(0, 8)
    def _(i):
        block = at(offset_at(i), 4)
        arrived(block)
        send(block, 64 + 56 + i, partner)

    @pl.loop(0, 64)
    def _(k):
        arrived(2 * k + 1 - core)

    @pl.loop(1, 128)
    def _(k):
        copy_of(ep, k, partner).wait_send()


def gather_weights(w_query, w_key, w_value, w_out_t):
    rows, cols = w_query.shape
    return pl.pallas_call(
        gather_kernel,
        out_shape=jax.ShapeDtypeStruct((4, 128, rows, cols), jnp.bfloat16),
        in_specs=[pl.BlockSpec(memory_space=pl.ANY)] * 4,
        out_specs=pl.BlockSpec(memory_space=pltpu.VMEM),
        scratch_shapes=[
            pltpu.SemaphoreType.DMA((4,)),
            pltpu.SemaphoreType.DMA((128,)),
            pltpu.SemaphoreType.DMA((128,)),
        ],
        compiler_params=pltpu.CompilerParams(collective_id=0, has_side_effects=True),
    )(w_query, w_key, w_value, w_out_t)


def sent_together(arrays, axis, dim, along):
    widths = [a.shape[along] for a in arrays]
    both = jnp.concatenate(arrays, axis=along)
    out = lax.all_gather(both, axis, axis=dim, tiled=True)
    return tuple(jnp.split(out, [sum(widths[:k]) for k in range(1, len(widths))], axis=along))


def from_everyone(array, axis):
    copies = jnp.broadcast_to(array, (lax.axis_size(axis), *array.shape))
    return lax.all_to_all(copies, axis, split_axis=0, concat_axis=0, tiled=True)


def taken_together(array, axis):
    everything = from_everyone(array, axis)
    return jnp.sum(everything.astype(jnp.float32), axis=0)


def split_up(array, dim, peers):
    before, after = (array.shape[:dim], array.shape[dim + 1 :])
    return jnp.moveaxis(array.reshape(*before, peers, -1, *after), dim, 0)


def sum_at_owner(array, axis, dim):
    peers = lax.axis_size(axis)
    parts = lax.all_to_all(split_up(array, dim, peers), axis, 0, 0, tiled=True)
    return jnp.sum(parts.astype(jnp.float32), axis=0)


def rms_scale(activity, gain):
    widened = activity.astype(jnp.float32)
    scaled = widened * lax.rsqrt(jnp.mean(widened * widened, axis=-1, keepdims=True) + norm_eps)
    return (scaled * gain).astype(jnp.bfloat16)


def low_rank(normed, decay_down, decay_up, decay_base, rate_down, rate_up):
    decay_low = jnp.tanh(jnp.dot(normed, decay_down, preferred_element_type=jnp.float32)).astype(
        jnp.bfloat16
    )
    decay_pre = decay_base + jnp.dot(decay_low, decay_up, preferred_element_type=jnp.float32)
    decays = jnp.exp(-jnp.exp(-jax.nn.softplus(-decay_pre) - 0.5))
    rate_low = jnp.dot(normed, rate_down, preferred_element_type=jnp.float32).astype(jnp.bfloat16)
    rates = jax.nn.sigmoid(jnp.dot(rate_low, rate_up, preferred_element_type=jnp.float32))
    return (decays, rates)


def recurrence(queries, key_rows, value_rows, decays, rates, old_state, head_gain):
    row_count, head_count, _ = old_state.shape
    head_size = queries.shape[1] // head_count
    head_shape = (row_count, head_count, head_size)
    query_heads = queries.astype(jnp.float32).reshape(head_shape)
    key_heads = key_rows.astype(jnp.float32).reshape(head_shape)
    value_heads = value_rows.astype(jnp.float32).reshape(head_shape)
    decay_heads = decays.reshape(head_shape)
    rate_heads = rates.reshape(head_shape)
    unit_keys = key_heads * lax.rsqrt(jnp.sum(key_heads * key_heads, axis=-1, keepdims=True) + 1.0)
    state_grid = old_state.reshape(row_count, head_count, head_size, head_size)
    removed = jnp.sum(state_grid * unit_keys[:, :, None, :], axis=-1)
    updated = (
        state_grid * decay_heads[:, :, None, :]
        - removed[:, :, :, None] * (unit_keys * rate_heads)[:, :, None, :]
        + value_heads[:, :, :, None] * key_heads[:, :, None, :]
    )
    readout = jnp.sum(updated * query_heads[:, :, None, :], axis=-1)
    centred = readout - jnp.mean(readout, axis=-1, keepdims=True)
    spread = jnp.mean(centred * centred, axis=-1, keepdims=True)
    scaled = centred * lax.rsqrt(spread + group_eps) * head_gain.reshape(head_count, head_size)
    return (
        updated.reshape(row_count, head_count, head_size * head_size),
        scaled.reshape(row_count, head_count * head_size).astype(jnp.bfloat16),
    )


def body(
    tokens,
    head_state,
    mixer_gain,
    w_query,
    w_key,
    w_value,
    decay_down,
    decay_up,
    decay_base,
    rate_down,
    rate_up,
    head_gain,
    w_out,
    expert_gain,
    expert_ids,
    route_weight,
    w_gate,
    w_up,
    w_down,
):
    seq_rows, width = tokens.shape
    local_cols = w_query.shape[1]
    head_lane = lax.axis_index("tp")
    normed = rms_scale(tokens, mixer_gain)
    gathered = gather_weights(w_query, w_key, w_value, w_out.T)
    full = gathered.reshape(4, width, local_cols)
    pieces = (full[0], full[1], full[2])
    projected = tuple(
        (
            jnp.dot(normed, weight_piece, preferred_element_type=jnp.float32)
            for weight_piece in pieces
        )
    )
    queries, key_rows, value_rows = (member.astype(jnp.bfloat16) for member in projected)
    col_offset = head_lane * local_cols
    decays, rates = low_rank(
        normed,
        decay_down,
        lax.dynamic_slice_in_dim(decay_up, col_offset, local_cols, 1),
        decay_base,
        rate_down,
        lax.dynamic_slice_in_dim(rate_up, col_offset, local_cols, 1),
    )
    next_state, head_out = recurrence(
        queries, key_rows, value_rows, decays, rates, head_state, head_gain
    )
    partial_out = lax.dot_general(
        head_out, full[3], (((1,), (1,)), ((), ())), preferred_element_type=jnp.float32
    )
    mixed_out = taken_together(partial_out.astype(jnp.bfloat16), "tp").astype(jnp.float32)
    residual = (tokens.astype(jnp.float32) + mixed_out).astype(jnp.bfloat16)
    expert_in = rms_scale(residual, expert_gain)
    experts = lax.axis_size("ep")
    top_count = expert_ids.shape[1]
    slot_count = max(1, 2 * seq_rows * top_count // experts)
    slot_total = experts * slot_count
    flat_ids = expert_ids.reshape(-1)
    matches = (flat_ids[:, None] == jnp.arange(experts, dtype=jnp.int32)[None, :]).astype(jnp.int32)
    slot_rank = jnp.sum((jnp.cumsum(matches, axis=0) - 1) * matches, axis=1)
    slot_ids = (flat_ids * slot_count + slot_rank).reshape(seq_rows, top_count)
    slot_match = (
        slot_ids[:, :, None] == jnp.arange(slot_total, dtype=jnp.int32)[None, None, :]
    ).astype(jnp.float32)
    picker = jnp.sum(slot_match, axis=1).astype(jnp.bfloat16)
    outbound = jnp.einsum("ts,td->sd", picker, expert_in, preferred_element_type=jnp.float32)
    outbound = outbound.astype(jnp.bfloat16).reshape(experts, slot_count, expert_in.shape[1])
    gate_local, up_local, down_local = (w_gate[0], w_up[0], w_down[0])
    arrived = lax.all_to_all(outbound, "ep", split_axis=0, concat_axis=0, tiled=True)
    sources, held, _ = arrived.shape
    flat_rows = arrived.reshape(sources * held, width)
    gate_act = jnp.dot(flat_rows, gate_local, preferred_element_type=jnp.float32)
    up_act = jnp.dot(flat_rows, up_local, preferred_element_type=jnp.float32)
    hidden = (jax.nn.silu(gate_act) * up_act).astype(jnp.bfloat16)
    partial_rows = jnp.dot(hidden, down_local, preferred_element_type=jnp.float32).reshape(
        sources, held, width
    )
    reduced = sum_at_owner(partial_rows.astype(jnp.bfloat16), "tp", 2)
    returned = lax.all_to_all(
        reduced.astype(jnp.bfloat16), "ep", split_axis=0, concat_axis=0, tiled=True
    )
    shares = route_weight / jnp.sum(route_weight, axis=1, keepdims=True)
    combine = jnp.sum(slot_match * shares[:, :, None], axis=1)
    routed = jnp.dot(combine, returned.reshape(slot_total, -1).astype(jnp.float32))
    own_cols = routed.shape[1]
    kept = lax.dynamic_slice_in_dim(residual, head_lane * own_cols, own_cols, 1)
    layer_out = (kept.astype(jnp.float32) + routed).astype(jnp.bfloat16)
    return (layer_out, next_state)


def solution(mesh):
    return jax.shard_map(
        body,
        mesh=mesh,
        in_specs=(
            P("ep", None),
            P("ep", "tp", None),
            P(),
            P("ep", "tp"),
            P("ep", "tp"),
            P("ep", "tp"),
            P(),
            P(),
            P("tp"),
            P(),
            P(),
            P("tp"),
            P("tp", "ep"),
            P(),
            P("ep", None),
            P("ep", None),
            P("ep", None, "tp"),
            P("ep", None, "tp"),
            P("ep", "tp", None),
        ),
        out_specs=(P("ep", "tp"), P("ep", "tp", None)),
        check_vma=False,
    )
```
